32 devices in a mesh: rep: 2 (over x), fs: 8 (over z, y), tp: 2 (over core).
Axes of the slice: x: 2, y: 2, z: 4, core: 2. Of those that a mesh axis runs over, the one named last changes fastest.
Arguments:
- hidden_in: bfloat16 [12288, 2048], P(('rep', 'fs', 'tp')), may hold values from -6 to 6
- norm_gain: float32 [2048], replicated, may hold values from 0.1 to 1.9
- up_weight: float32 [2048, 8192], P('fs', 'tp'), may hold values from -0.125 to 0.125
- up_scale: float32 [8192], P('tp'), may hold values from 0.5 to 2
- down_weight: float32 [8192, 2048], P('tp', 'fs'), may hold values from -0.0625 to 0.0625
- down_scale: float32 [2048], replicated, may hold values from 0.5 to 2
Outputs:
- layer_out: bfloat16 [12288, 2048], P(('rep', 'fs', 'tp'))
The draws below stay inside these ranges and needn't reach their ends.
All inputs are finite; a program needn't handle non-finite values.
Results may differ from the reference program's by a relative error of at most 0.0085.
Values may be sent and summed in bfloat16 or wider, within the bound.
A program may use at most 128 MiB of HBM per device.

```python
import math
import jax
import jax.numpy as jnp
from jax import lax

D = 2048
FF = 8192
TOKENS = 12288
N_TP = 2


def shard_levels(rng, shape, split, smallest, high):
    def one(dim, parts):
        draws = jax.random.uniform(jax.random.fold_in(jax.random.fold_in(rng, 6), dim), (parts,), jnp.float32, smallest / len(split), high / len(split))
        return jnp.repeat(jnp.exp(draws), shape[dim] // parts).reshape((-1,) + (1,) * (len(shape) - dim - 1))

    level = one(*split[0])
    for cut in split[1:]:
        level = level * one(*cut)
    return level


def normal_values(stream_key, shape, deviation, most, pieces=(), kind=jnp.bfloat16):
    level = shard_levels(stream_key, shape, pieces, -0.22, 0.18) if pieces else 1.0
    values = jax.random.normal(stream_key, shape, jnp.float32) * deviation * level
    return jnp.minimum(jnp.maximum(values, -most), most).astype(kind)


def setup_inputs(seed: int = 0) -> dict:
    seeds = jax.random.split(jax.random.key(seed), 7)
    return {
        "hidden_in": normal_values(seeds[0], (TOKENS, D), 1.0, 6.0, ((0, 32),)),
        "norm_gain": jnp.clip(1.0 + 0.18 * jax.random.normal(seeds[1], (D,), jnp.float32), 0.1, 1.9),
        "up_weight": normal_values(seeds[2], (D, FF), D ** -0.5, 0.125, ((0, 8), (1, 2)), jnp.float32),
        "up_scale": jnp.clip(jnp.exp(math.log(2.0) - 1.3862944 * jax.random.uniform(seeds[3], (FF,), jnp.float32) ** shard_levels(seeds[3], (FF,), ((0, 2),), -0.2, 0.2)), 0.5, 2.0),
        "down_weight": normal_values(seeds[4], (FF, D), FF ** -0.5, 0.0625, ((0, 2), (1, 8)), jnp.float32),
        "down_scale": jnp.clip(jnp.exp(jax.random.uniform(seeds[5], (D,), jnp.float32, math.log(0.5), math.log(2.0))), 0.5, 2.0),
    }


def reference(hidden_in, norm_gain, up_weight, up_scale, down_weight, down_scale):
    up_low = up_weight.astype(jnp.bfloat16)
    down_low = down_weight.astype(jnp.bfloat16)
    block = math.gcd(2048, TOKENS)
    width = FF // N_TP

    def one_block(start):
        rows = lax.dynamic_slice_in_dim(hidden_in, start, block, 0).astype(jnp.float32)
        normed = (rows * lax.rsqrt(lax.optimization_barrier(jnp.mean(rows * rows, axis=1, keepdims=True)) + 1e-06) * norm_gain).astype(jnp.bfloat16)
        pre = jnp.dot(normed, up_low, preferred_element_type=jnp.float32) * up_scale
        act = jnp.square(jnp.maximum(pre, 0.0)).astype(jnp.bfloat16)
        total = jnp.zeros((block, D), jnp.float32)
        for index in range(N_TP):
            part = jnp.dot(act[:, index * width:(index + 1) * width], down_low[index * width:(index + 1) * width], preferred_element_type=jnp.float32).astype(jnp.bfloat16)
            part = lax.optimization_barrier(part)
            total = total + part.astype(jnp.float32)
        return (total * down_scale).astype(jnp.bfloat16)
    starts = jnp.arange(0, TOKENS, block, dtype=jnp.int32)
    outs = lax.map(one_block, starts)
    return outs.reshape(TOKENS, D)
```

```python
import jax
import jax.numpy as jnp
from jax import lax
from jax.sharding import Mesh, PartitionSpec as P


def body(hidden_in, norm_gain, up_weight, up_scale, down_weight, down_scale):
    rep, pair = lax.axis_index("rep"), lax.axis_index("fy")
    n_rep, n_pair = lax.axis_size("rep"), lax.axis_size("fy")
    group = ("rep", "fy", "tp")
    units = up_weight.shape[1] // n_rep

    rows = hidden_in.astype(jnp.float32)
    normed = (
        rows * lax.rsqrt(jnp.mean(rows * rows, axis=1, keepdims=True) + 1e-06) * norm_gain
    ).astype(jnp.bfloat16)
    up_low = lax.dynamic_slice_in_dim(up_weight, rep * units, units, 1).astype(jnp.bfloat16)
    up_pair = lax.all_to_all(up_low, "fy", 1, 0, tiled=True)
    up_whole = lax.all_gather(up_pair, "fz", axis=0, tiled=True)
    gathered = lax.all_gather(normed, group, axis=0, tiled=True)
    down_low = lax.dynamic_slice_in_dim(down_weight, rep * units, units, 0).astype(jnp.bfloat16)
    down_pair = lax.all_to_all(down_low, "fy", 0, 1, tiled=True)
    down_whole = lax.all_gather(down_pair, "fz", axis=1, tiled=True)
    width = units // n_pair
    scale = lax.dynamic_slice_in_dim(up_scale, (rep * n_pair + pair) * width, width, 0)
    pre = jnp.dot(gathered, up_whole, preferred_element_type=jnp.float32)
    act = jnp.square(jnp.maximum(pre * scale, 0.0)).astype(jnp.bfloat16)
    summed = lax.psum_scatter(
        jnp.dot(act, down_whole, preferred_element_type=jnp.float32).astype(jnp.bfloat16),
        group,
        scatter_dimension=0,
        tiled=True,
    ).astype(jnp.float32)
    return (summed * down_scale).astype(jnp.bfloat16)


def solution(mesh):
    n_rep, n_fs, n_tp = (mesh.shape[a] for a in ("rep", "fs", "tp"))
    pair = 2 if n_fs % 2 == 0 else 1
    split = Mesh(
        mesh.devices.reshape(n_rep, n_fs // pair, pair, n_tp), ("rep", "fz", "fy", "tp")
    )
    fs = ("fz", "fy")
    tokens = P(("rep", *fs, "tp"), None)
    placed = (tokens, P(), P(fs, "tp"), P("tp"), P("tp", fs), P())
    return jax.shard_map(body, mesh=split, in_specs=placed, out_specs=tokens, check_vma=False)
```

```python
import functools

import jax
import jax.numpy as jnp
from jax import lax
from jax.experimental import pallas as pl
from jax.experimental.pallas import tpu as pltpu
from jax.sharding import Mesh, PartitionSpec as P

MESH = pl.DeviceIdType.MESH


def kernel(
    n, normed, up_own, up_peer, dn_own, dn_peer, up_scale, dn_scale, out,
    tok, up_w, dn_w, act, psend, precv, csum, ra1, rb1, ra2, rb2, ss, rs, ls,
):
    x, z, y, c = (lax.axis_index(a) for a in ("rep", "fz", "fy", "tp"))
    ox, oy, oc = 1 - x, 1 - y, 1 - c
    right, left = lax.rem(z + 1, n), lax.rem(z + n - 1, n)
    to_x, to_y, to_c = {"rep": ox}, {"fy": oy}, {"tp": oc}
    to_right, to_left = {"fz": right}, {"fz": left}
    kr, width = up_own.shape
    rows, depth = normed.shape
    half = depth // 2
    top = rows // 2

    barrier = pltpu.get_barrier_semaphore()
    for other in (to_x, to_y, to_c, to_right, to_left):
        pl.semaphore_signal(barrier, inc=1, device_id=other, device_id_type=MESH)
    pl.semaphore_wait(barrier, 5)

    copies = []

    def send(src, dst, other):
        i = len(copies)
        copy = pltpu.make_async_remote_copy(
            src_ref=src, dst_ref=dst, send_sem=ss.at[i], recv_sem=rs.at[i],
            device_id=other, device_id_type=MESH,
        )
        copy.start()
        copies.append(copy)
        return copy

    def up_at(zz, yy):
        return up_w.at[pl.ds(pl.multiple_of((zz * 2 + yy) * kr, kr), kr)]

    def dn_at(zz, yy):
        return dn_w.at[zz * 2 + yy]

    ring = {}

    def hop(step, yy, chain):
        if step == 0 and chain == 0:
            u_src, d_src = up_own, dn_own
        else:
            u_src = up_at(lax.rem(z - step + n, n), yy)
            d_src = dn_at(lax.rem(z + step, n), yy)
        ring[chain, step] = (
            send(u_src, up_at(lax.rem(z - step + n, n), yy), to_right),
            send(d_src, dn_at(lax.rem(z + step, n), yy), to_left),
        )

    def arrived(step, chain):
        for copy in ring[chain, step]:
            copy.wait_recv()

    hop(0, y, 0)
    y_up = send(up_peer, up_at(z, y), to_y)
    y_dn = send(dn_peer, dn_at(z, y), to_y)
    tx = send(normed, tok.at[c, x, y], to_x)
    ty = send(normed, tok.at[c, x, y], to_y)
    tc = send(normed, tok.at[c, x, y], to_c)
    mine = (
        pltpu.make_async_copy(up_own, up_at(z, y), ls.at[0]),
        pltpu.make_async_copy(dn_own, dn_at(z, y), ls.at[1]),
        pltpu.make_async_copy(normed, tok.at[c, x, y], ls.at[2]),
    )
    for copy in mine:
        copy.start()

    arrived(0, 0)
    hop(1, y, 0)
    y_up.wait_recv()
    y_dn.wait_recv()
    hop(0, oy, 1)
    for step in range(1, n - 2):
        arrived(step, 0)
        hop(step + 1, y, 0)
    tx.wait_recv()
    diag_y = send(tok.at[c, ox, y, pl.ds(0, top)], tok.at[c, ox, y, pl.ds(0, top)], to_y)
    cx = send(tok.at[c, ox, y], tok.at[c, ox, y], to_c)
    arrived(0, 1)
    hop(1, oy, 1)
    ty.wait_recv()
    diag_x = send(tok.at[c, x, oy, pl.ds(top, top)], tok.at[c, x, oy, pl.ds(top, top)], to_x)
    cy = send(tok.at[c, x, oy], tok.at[c, x, oy], to_c)
    for step in range(1, n - 2):
        arrived(step, 1)
        hop(step + 1, oy, 1)
    diag_y.wait_recv()
    diag_x.wait_recv()
    cd = send(tok.at[c, ox, oy], tok.at[c, ox, oy], to_c)
    arrived(n - 2, 0)
    arrived(n - 2, 1)
    for copy in (tc, cx, cy, cd):
        copy.wait_recv()
    for copy in mine:
        copy.wait()

    tile = min(256, width)
    n_fs, _, cols = dn_w.shape
    per_half = n_fs // 2

    def hidden(cc, xx, yy):
        @pl.loop(0, width // tile)
        def _(i):
            at = pl.ds(pl.multiple_of(i * tile, tile), tile)
            pre = jnp.dot(tok[cc, xx, yy], up_w[:, at], preferred_element_type=jnp.float32)
            act[:, at] = jnp.square(jnp.maximum(pre * up_scale[:, at], 0.0)).astype(jnp.bfloat16)

    def each_slot(emit):
        for h in range(2):
            def one(s, at):
                part = jnp.dot(
                    act[...], dn_w[h * per_half + s], preferred_element_type=jnp.float32
                )
                emit(h, at, part.astype(jnp.bfloat16))

            if cols % 128 == 0:
                @pl.loop(0, per_half)
                def _(s):
                    one(s, pl.ds(pl.multiple_of(s * cols, cols), cols))
            else:
                for s in range(per_half):
                    one(s, pl.ds(s * cols, cols))

    def for_partner(xx, yy):
        hidden(oc, xx, yy)

        def emit(h, at, part):
            psend[xx, yy, h, :, at] = part

        each_slot(emit)
        return send(psend.at[xx, yy], precv.at[xx, yy], to_c)

    def for_own(xx, yy, got):
        hidden(c, xx, yy)
        got.wait_recv()

        def emit(h, at, part):
            total = part.astype(jnp.float32) + precv[xx, yy, h, :, at].astype(jnp.float32)
            csum[xx, yy, h, :, at] = total.astype(jnp.bfloat16)

        each_slot(emit)

    def add(xx, yy, h, got):
        total = csum[xx, yy, h].astype(jnp.float32) + got[...].astype(jnp.float32)
        csum[xx, yy, h] = total.astype(jnp.bfloat16)

    p_diag = for_partner(ox, oy)
    p_x = for_partner(ox, y)
    for_own(ox, oy, p_diag)
    a_diag = send(csum.at[ox, oy, 0], ra1.at[oy], to_x)
    b_diag = send(csum.at[ox, oy, 1], rb1.at[ox], to_y)
    p_y = for_partner(x, oy)
    for_own(ox, y, p_x)
    a_x = send(csum.at[ox, y, 0], ra1.at[y], to_x)
    p_own = for_partner(x, y)
    for_own(x, oy, p_y)
    b_y = send(csum.at[x, oy, 1], rb1.at[x], to_y)
    a_diag.wait_recv()
    add(x, oy, 0, ra1.at[oy])
    a_last = send(csum.at[x, oy, 0], ra2, to_y)
    b_diag.wait_recv()
    add(ox, y, 1, rb1.at[ox])
    b_last = send(csum.at[ox, y, 1], rb2, to_x)
    for_own(x, y, p_own)
    a_x.wait_recv()
    b_y.wait_recv()
    a_last.wait_recv()
    b_last.wait_recv()
    for h, first, last in ((0, ra1.at[y], ra2), (1, rb1.at[x], rb2)):
        at = pl.ds(h * half, half)
        total = csum[x, y, h].astype(jnp.float32) + first[...].astype(jnp.float32)
        total = total + last[...].astype(jnp.float32)
        out[:, at] = (total * dn_scale[:, at]).astype(out.dtype)
    for copy in copies:
        copy.wait_send()


def body(hidden_in, norm_gain, up_weight, up_scale, down_weight, down_scale):
    rep, pair = lax.axis_index("rep"), lax.axis_index("fy")
    n = lax.axis_size("fz")
    width = up_weight.shape[1] // 4
    rows, depth = hidden_in.shape
    kr, cols = up_weight.shape[0], down_weight.shape[1]

    wide = hidden_in.astype(jnp.float32)
    normed = (
        wide * lax.rsqrt(jnp.mean(wide * wide, axis=1, keepdims=True) + 1e-06) * norm_gain
    ).astype(jnp.bfloat16)

    def cut(array, dim, yy):
        return lax.dynamic_slice_in_dim(array, (rep * 2 + yy) * width, width, dim)

    low = jnp.bfloat16
    half = depth // 2
    sends = 4 * (n - 1) + 20
    vmem = pl.BlockSpec(memory_space=pltpu.VMEM)
    return pl.pallas_call(
        functools.partial(kernel, n),
        out_shape=jax.ShapeDtypeStruct((rows, depth), low),
        in_specs=[vmem] * 7,
        out_specs=vmem,
        scratch_shapes=[
            pltpu.VMEM((2, 2, 2, rows, depth), low),
            pltpu.VMEM((2 * n * kr, width), low),
            pltpu.VMEM((2 * n, width, cols), low),
            pltpu.VMEM((rows, width), low),
            pltpu.VMEM((2, 2, 2, rows, half), low),
            pltpu.VMEM((2, 2, 2, rows, half), low),
            pltpu.VMEM((2, 2, 2, rows, half), low),
            pltpu.VMEM((2, rows, half), low),
            pltpu.VMEM((2, rows, half), low),
            pltpu.VMEM((rows, half), low),
            pltpu.VMEM((rows, half), low),
            pltpu.SemaphoreType.DMA((sends,)),
            pltpu.SemaphoreType.DMA((sends,)),
            pltpu.SemaphoreType.DMA((3,)),
        ],
        compiler_params=pltpu.CompilerParams(
            collective_id=0, has_side_effects=True, vmem_limit_bytes=60 * 1024 * 1024
        ),
    )(
        normed,
        cut(up_weight, 1, pair).astype(low),
        cut(up_weight, 1, 1 - pair).astype(low),
        cut(down_weight, 0, pair).astype(low),
        cut(down_weight, 0, 1 - pair).astype(low),
        cut(up_scale, 0, pair).reshape(1, width),
        down_scale.reshape(1, depth),
    )


def solution(mesh):
    n_rep, n_fs, n_tp = (mesh.shape[a] for a in ("rep", "fs", "tp"))
    split = Mesh(mesh.devices.reshape(n_rep, n_fs // 2, 2, n_tp), ("rep", "fz", "fy", "tp"))
    fs = ("fz", "fy")
    tokens = P(("rep", *fs, "tp"), None)
    placed = (tokens, P(), P(fs, "tp"), P("tp"), P("tp", fs), P())
    return jax.shard_map(body, mesh=split, in_specs=placed, out_specs=tokens, check_vma=False)
```

```python
import functools

import jax
import jax.numpy as jnp
from jax import lax
from jax.experimental import pallas as pl
from jax.experimental.pallas import tpu as pltpu
from jax.sharding import Mesh, PartitionSpec as P

MESH = pl.DeviceIdType.MESH


def kernel(
    n, normed, up_own, up_peer, dn_own, dn_peer, up_scale, dn_scale, out,
    tok, up_w, dn_w, act, psend, precv, csum, ra1, rb1, ra2, rb2, ss, rs, ls,
):
    x, z, y, c = (lax.axis_index(a) for a in ("rep", "fz", "fy", "tp"))
    ox, oy, oc = 1 - x, 1 - y, 1 - c
    right, left = lax.rem(z + 1, n), lax.rem(z + n - 1, n)
    to_x, to_y, to_c = {"rep": ox}, {"fy": oy}, {"tp": oc}
    to_right, to_left = {"fz": right}, {"fz": left}
    kr, width = up_own.shape
    rows, depth = normed.shape
    cols = dn_own.shape[1]
    top, part_rows = rows // 2, kr // 2

    barrier = pltpu.get_barrier_semaphore()
    for other in (to_x, to_y, to_c, to_right, to_left):
        pl.semaphore_signal(barrier, inc=1, device_id=other, device_id_type=MESH)
    pl.semaphore_wait(barrier, 5)

    count = [0]

    def send(src, dst, other):
        i = count[0]
        count[0] += 1
        copy = pltpu.make_async_remote_copy(
            src_ref=src, dst_ref=dst, send_sem=ss.at[i], recv_sem=rs.at[i],
            device_id=other, device_id_type=MESH,
        )
        copy.start()
        return copy

    def up_at(zz, yy, h):
        start = (zz * 2 + yy) * kr + h * part_rows
        return up_w.at[pl.ds(pl.multiple_of(start, part_rows), part_rows)]

    ups, downs = {}, {}

    def up_hop(step, yy, chain):
        pair = []
        for h, other in ((0, to_right), (1, to_left)):
            owner = lax.rem(z - step + n, n) if h == 0 else lax.rem(z + step, n)
            dst = up_at(owner, yy, h)
            first = step == 0 and chain == 0
            pair.append(send(up_own.at[pl.ds(h * part_rows, part_rows)] if first else dst, dst, other))
        ups[chain, step] = pair

    def up_arrived(step, chain):
        for copy in ups[chain, step]:
            copy.wait_recv()

    def slots(k):
        return lax.rem(z - k + n, n) * 2, lax.rem(z + k, n) * 2 + 1

    def down_hop(step):
        one, two = (dn_w.at[s] for s in slots(step))
        downs[step] = send(one, one, to_right), send(two, two, to_left)

    up_hop(0, y, 0)
    here = pl.ds(pl.multiple_of((z * 2 + y) * kr, kr), kr)
    y_up = send(up_peer, up_w.at[here], to_y)
    y_dn = send(dn_peer, dn_w.at[z * 2 + y], to_y)
    tx = send(normed, tok.at[c, x, y], to_x)
    ty = send(normed, tok.at[c, x, y], to_y)
    tc = send(normed, tok.at[c, x, y], to_c)
    mine = (
        pltpu.make_async_copy(up_own, up_w.at[here], ls.at[0]),
        pltpu.make_async_copy(dn_own, dn_w.at[z * 2 + y], ls.at[1]),
        pltpu.make_async_copy(normed, tok.at[c, x, y], ls.at[2]),
    )
    for copy in mine:
        copy.start()

    up_arrived(0, 0)
    up_hop(1, y, 0)
    y_up.wait_recv()
    up_hop(0, oy, 1)
    for step in range(1, n - 2):
        up_arrived(step, 0)
        up_hop(step + 1, y, 0)
    up_arrived(0, 1)
    up_hop(1, oy, 1)
    tx.wait_recv()
    diag_y = send(tok.at[c, ox, y, pl.ds(0, top)], tok.at[c, ox, y, pl.ds(0, top)], to_y)
    cx = send(tok.at[c, ox, y], tok.at[c, ox, y], to_c)
    for step in range(1, n - 2):
        up_arrived(step, 1)
        up_hop(step + 1, oy, 1)
    for copy in mine:
        copy.wait()
    y_dn.wait_recv()
    down_hop(0)
    ty.wait_recv()
    diag_x = send(tok.at[c, x, oy, pl.ds(top, top)], tok.at[c, x, oy, pl.ds(top, top)], to_x)
    cy = send(tok.at[c, x, oy], tok.at[c, x, oy], to_c)
    up_arrived(n - 2, 0)
    up_arrived(n - 2, 1)
    diag_y.wait_recv()
    diag_x.wait_recv()
    cd = send(tok.at[c, ox, oy], tok.at[c, ox, oy], to_c)
    for copy in (tc, cx, cy, cd):
        copy.wait_recv()

    tile = min(256, width)

    @pl.loop(0, 8)
    def _(i):
        cc, xx, yy = i // 4, (i // 2) % 2, i % 2

        @pl.loop(0, width // tile)
        def _(j):
            at = pl.ds(pl.multiple_of(j * tile, tile), tile)
            pre = jnp.dot(tok[cc, xx, yy], up_w[:, at], preferred_element_type=jnp.float32)
            act[cc, xx, yy, :, at] = jnp.square(
                jnp.maximum(pre * up_scale[:, at], 0.0)
            ).astype(jnp.bfloat16)

    def each_part(k, cc, emit):
        one, two = slots(k)

        @pl.loop(0, 8)
        def _(i):
            h, f, s = i // 4, (i // 2) % 2, i % 2
            xx, yy = f + h * (s - f), s + h * (f - s)
            part = jnp.dot(
                act[cc, xx, yy], dn_w[one + h * (two - one)], preferred_element_type=jnp.float32
            )
            emit(h, f, s, part.astype(jnp.bfloat16))

    given, first, last = {}, {}, {}

    def for_partner(k):
        p = k % 2
        if k >= 2:
            given[k - 2].wait_send()

        def emit(h, f, s, part):
            psend[p, h, f, s] = part

        each_part(k, oc, emit)
        given[k] = send(psend.at[p], precv.at[k], to_c)

    def for_own(k):
        p = k % 2
        given[k].wait_recv()

        def emit(h, f, s, part):
            total = part.astype(jnp.float32) + precv[k, h, f, s].astype(jnp.float32)
            csum[p, h, f, s] = total.astype(jnp.bfloat16)

        each_part(k, c, emit)
        first[k] = (
            send(csum.at[p, 0, ox], ra1.at[k], to_x),
            send(csum.at[p, 1, oy], rb1.at[k], to_y),
        )

    def second_stage(k):
        p = k % 2
        sent = []
        for h, f, s, got, dst, other in (
            (0, x, oy, ra1, ra2, to_y), (1, y, ox, rb1, rb2, to_x)
        ):
            first[k][h].wait_recv()
            total = csum[p, h, f, s].astype(jnp.float32) + got[k, s].astype(jnp.float32)
            csum[p, h, f, s] = total.astype(jnp.bfloat16)
            sent.append(send(csum.at[p, h, f, s], dst.at[k], other))
        last[k] = sent

    def finish(k):
        p = k % 2
        for h, f, s, one, two in ((0, x, y, ra1, ra2), (1, y, x, rb1, rb2)):
            last[k][h].wait_recv()
            total = csum[p, h, f, s].astype(jnp.float32) + one[k, s].astype(jnp.float32)
            total = total + two[k].astype(jnp.float32)
            slot = slots(k)[h]
            value = (total * dn_scale[slot]).astype(out.dtype)
            if cols % 128 == 0:
                out[:, pl.ds(pl.multiple_of(slot * cols, cols), cols)] = value
            else:
                out[slot] = value
        for copy in (*first[k], *last[k]):
            copy.wait_send()

    for k in range(n):
        if k >= 1:
            for copy in downs[k - 1]:
                copy.wait_recv()
            if k < n - 1:
                down_hop(k)
        for_partner(k)
        if k >= 1:
            second_stage(k - 1)
        if k >= 2:
            finish(k - 2)
        for_own(k)
    second_stage(n - 1)
    finish(n - 2)
    finish(n - 1)
    for pair in (*ups.values(), *downs.values()):
        for copy in pair:
            copy.wait_send()
    for copy in (y_up, y_dn, tx, ty, tc, diag_y, cx, diag_x, cy, cd, given[n - 2], given[n - 1]):
        copy.wait_send()


def body(hidden_in, norm_gain, up_weight, up_scale, down_weight, down_scale):
    rep, pair = lax.axis_index("rep"), lax.axis_index("fy")
    n = lax.axis_size("fz")
    width = up_weight.shape[1] // 4
    rows, depth = hidden_in.shape
    kr, cols = up_weight.shape[0], down_weight.shape[1]

    wide = hidden_in.astype(jnp.float32)
    normed = (
        wide * lax.rsqrt(jnp.mean(wide * wide, axis=1, keepdims=True) + 1e-06) * norm_gain
    ).astype(jnp.bfloat16)

    def cut(array, dim, yy):
        return lax.dynamic_slice_in_dim(array, (rep * 2 + yy) * width, width, dim)

    low = jnp.bfloat16
    sends = 6 * (n - 1) + 10 + 5 * n
    flat = cols % 128 == 0
    vmem = pl.BlockSpec(memory_space=pltpu.VMEM)
    made = pl.pallas_call(
        functools.partial(kernel, n),
        out_shape=jax.ShapeDtypeStruct((rows, depth) if flat else (2 * n, rows, cols), low),
        in_specs=[vmem] * 7,
        out_specs=vmem,
        scratch_shapes=[
            pltpu.VMEM((2, 2, 2, rows, depth), low),
            pltpu.VMEM((2 * n * kr, width), low),
            pltpu.VMEM((2 * n, width, cols), low),
            pltpu.VMEM((2, 2, 2, rows, width), low),
            pltpu.VMEM((2, 2, 2, 2, rows, cols), low),
            pltpu.VMEM((n, 2, 2, 2, rows, cols), low),
            pltpu.VMEM((2, 2, 2, 2, rows, cols), low),
            pltpu.VMEM((n, 2, rows, cols), low),
            pltpu.VMEM((n, 2, rows, cols), low),
            pltpu.VMEM((n, rows, cols), low),
            pltpu.VMEM((n, rows, cols), low),
            pltpu.SemaphoreType.DMA((sends,)),
            pltpu.SemaphoreType.DMA((sends,)),
            pltpu.SemaphoreType.DMA((3,)),
        ],
        compiler_params=pltpu.CompilerParams(
            collective_id=0, has_side_effects=True, vmem_limit_bytes=60 * 1024 * 1024
        ),
    )(
        normed,
        cut(up_weight, 1, pair).astype(low),
        cut(up_weight, 1, 1 - pair).astype(low),
        cut(down_weight, 0, pair).astype(low),
        cut(down_weight, 0, 1 - pair).astype(low),
        cut(up_scale, 0, pair).reshape(1, width),
        down_scale.reshape(2 * n, 1, cols),
    )
    return made if flat else made.transpose(1, 0, 2).reshape(rows, depth)


def solution(mesh):
    n_rep, n_fs, n_tp = (mesh.shape[a] for a in ("rep", "fs", "tp"))
    split = Mesh(mesh.devices.reshape(n_rep, n_fs // 2, 2, n_tp), ("rep", "fz", "fy", "tp"))
    fs = ("fz", "fy")
    tokens = P(("rep", *fs, "tp"), None)
    placed = (tokens, P(), P(fs, "tp"), P("tp"), P("tp", fs), P())
    return jax.shard_map(body, mesh=split, in_specs=placed, out_specs=tokens, check_vma=False)
```
